32 devices in a mesh: sp: 16 (over z, y, x), tp: 2 (over core).
Axes of the slice: x: 2, y: 2, z: 4, core: 2. Of those that a mesh axis runs over, the one named last changes fastest.
Arguments:
- tokens: bfloat16 [4096, 2048], P('sp'), may hold values from -6 to 6
- query_weight: bfloat16 [2, 2048, 512], P(None, None, 'tp'), may hold values from -0.125 to 0.125
- key_weight: bfloat16 [2, 2048, 512], P(None, None, 'tp'), may hold values from -0.125 to 0.125
- value_weight: bfloat16 [2, 2048, 512], P(None, None, 'tp'), may hold values from -0.125 to 0.125
- out_weight: bfloat16 [2, 512, 2048], replicated, may hold values from -1.5 to 1.5
- rel_table: float32 [2, 8, 257], P(None, 'tp'), may hold values from -5 to 262
- norm_gain: float32 [2, 2048], replicated, may hold values from 0.1 to 1.9
- norm_bias: float32 [2, 2048], replicated, may hold values from -1.5 to 1.5
Outputs:
- encoded: bfloat16 [4096, 2048], P('sp', 'tp')
The draws below stay inside these ranges and needn't reach their ends.
All inputs are finite; a program needn't handle non-finite values.
Results may differ from the reference program's by a relative error of at most 0.0095.
Values may be sent and summed in bfloat16 or wider, within the bound.
A program may use at most 64 MiB of HBM per device.

```python
import jax
import jax.numpy as jnp
from jax import lax

D = 2048
HEADS = 8
HEAD_DIM = 64
SEG = 64
LEFT = 4
CLIP = 128
LAYERS = 2
HW = 512
TOKENS = 4096


def draw_rel_table(key, part):
    shape = (LAYERS, HEADS, 2 * CLIP + 1)
    return jnp.clip(jax.random.normal(key, shape, jnp.float32), -5.0, 5.0)


def block_scale(key, dims, split, low, largest):
    level, own = 1.0, jax.random.fold_in(key, 6)
    for position, parts in split:
        draws = jnp.exp(jax.random.uniform(jax.random.fold_in(own, position), (parts,), jnp.float32, low / len(split), largest / len(split)))
        level = level * jnp.repeat(draws, dims[position] // parts).reshape([-1 if axis == position else 1 for axis in range(len(dims))])
    return level


def gaussian(key, shape, scale, most, cuts=(), held_as=jnp.bfloat16):
    level = block_scale(key, shape, cuts, -0.22, 0.18) if cuts else 1.0
    values = jax.random.normal(key, shape, jnp.float32) * scale * level
    return jnp.minimum(jnp.maximum(values, -most), most).astype(held_as)


def setup_inputs(seed: int = 0) -> dict:
    seeds = jax.random.split(jax.random.key(seed), 9)
    return {
        "tokens": gaussian(seeds[0], (TOKENS, D), 1.0, 6.0, ((0, 16),)),
        "query_weight": gaussian(seeds[1], (LAYERS, D, HW), D ** -0.5, 0.125, ((2, 2),)),
        "key_weight": gaussian(seeds[2], (LAYERS, D, HW), D ** -0.5, 0.125, ((2, 2),)),
        "value_weight": gaussian(seeds[3], (LAYERS, D, HW), D ** -0.5, 0.125, ((2, 2),)),
        "out_weight": gaussian(seeds[4], (LAYERS, HW, D), (HW // 32) ** -0.5, 1.5),
        "rel_table": draw_rel_table(jax.random.fold_in(seeds[8], 71), 0),
        "norm_gain": jnp.clip(1.0 + 0.18 * jax.random.normal(seeds[6], (LAYERS, D), jnp.float32), 0.1, 1.9),
        "norm_bias": gaussian(seeds[7], (LAYERS, D), 0.3, 1.5, (), jnp.float32),
    }


residual_scale = 2.0 ** 0.5
norm_eps = 1e-05
masked_score = -1e+30

def post_norm(previous, mixed, gain, shift):
    total = residual_scale * previous.astype(jnp.float32) + mixed
    mean = lax.optimization_barrier(jnp.mean(total, -1, keepdims=True))
    centred = total - mean
    variance = lax.optimization_barrier(jnp.mean(centred * centred, -1, keepdims=True))
    return (centred * lax.rsqrt(variance + norm_eps) * gain + shift).astype(jnp.bfloat16)

def band_attention(query, keys, values, table):
    reach = LEFT * SEG
    band = reach + SEG
    seg_count = TOKENS // SEG
    query3 = query.reshape(TOKENS, HEADS, HEAD_DIM)
    zeros = jnp.zeros((reach, HEADS, HEAD_DIM), jnp.bfloat16)
    padded_keys = jnp.concatenate([zeros, keys.reshape(TOKENS, HEADS, HEAD_DIM)], axis=0)
    padded_values = jnp.concatenate([zeros, values.reshape(TOKENS, HEADS, HEAD_DIM)], axis=0)
    distance = reach + jnp.arange(SEG, dtype=jnp.int32)[:, None] - jnp.arange(band, dtype=jnp.int32)[None, :]
    column = jnp.clip(distance, -CLIP, CLIP) + CLIP
    bias = table.astype(jnp.float32)[:, column]

    def one_segment(index):
        start = (index * SEG).astype(jnp.int32)
        query_block = lax.dynamic_slice_in_dim(query3, start, SEG, 0).astype(jnp.float32)
        key_band = lax.dynamic_slice_in_dim(padded_keys, start, band, 0).astype(jnp.float32)
        value_band = lax.dynamic_slice_in_dim(padded_values, start, band, 0).astype(jnp.float32)
        scores = jnp.einsum('qhd,khd->hqk', query_block, key_band) * HEAD_DIM ** (-0.5) + bias
        key_position = start - reach + jnp.arange(band, dtype=jnp.int32)
        scores = jnp.where((key_position >= 0)[None, None, :], scores, masked_score)
        peak = lax.optimization_barrier(jnp.max(scores, -1, keepdims=True))
        expo = jnp.exp(scores - peak)
        weights = (expo / lax.optimization_barrier(jnp.sum(expo, -1, keepdims=True))).astype(jnp.bfloat16)
        attended = jnp.einsum('hqk,khd->qhd', weights.astype(jnp.float32), value_band)
        return attended.astype(jnp.bfloat16)
    blocks = lax.map(one_segment, jnp.arange(seg_count, dtype=jnp.int32))
    return blocks.reshape(TOKENS, HEADS * HEAD_DIM)

def reference(tokens, query_weight, key_weight, value_weight, out_weight, rel_table, norm_gain, norm_bias):
    hidden = tokens
    for layer_index in range(LAYERS):
        query = jnp.dot(hidden, query_weight[layer_index], preferred_element_type=jnp.float32).astype(jnp.bfloat16)
        keys = jnp.dot(hidden, key_weight[layer_index], preferred_element_type=jnp.float32).astype(jnp.bfloat16)
        values = jnp.dot(hidden, value_weight[layer_index], preferred_element_type=jnp.float32).astype(jnp.bfloat16)
        attended = band_attention(query, keys, values, rel_table[layer_index])
        mixed = jnp.dot(attended, out_weight[layer_index], preferred_element_type=jnp.float32)
        hidden = post_norm(hidden, mixed, norm_gain[layer_index], norm_bias[layer_index])
    return hidden
```

```python
import functools

import jax
import jax.numpy as jnp
from jax import lax
from jax.experimental import pallas as pl
from jax.experimental.pallas import tpu as pltpu
from jax.sharding import PartitionSpec as P

SEG = 64
LEFT = 4
CLIP = 128
LAYERS = 2
CHUNKS = 2
LANES = 128

residual_scale = 2.0**0.5
norm_eps = 1e-05
masked_score = -1e30
MESH = pl.DeviceIdType.MESH


def kernel(
    sp_count,
    heads,
    tokens,
    wq_hbm,
    wk_hbm,
    wv_hbm,
    wo_hbm,
    table,
    gain,
    shift,
    out,
    x0,
    x1,
    wq,
    wk,
    wv,
    wo,
    query,
    kx,
    vx,
    att,
    total,
    bias,
    padded,
    x_sem,
    w_sem,
    halo_send,
    halo_recv,
    pair_send,
    pair_recv,
):
    rows, model = x0.shape
    width = query.shape[1]
    head_size = width // heads
    reach = LEFT * SEG
    band = reach + SEG
    chunk = rows // CHUNKS
    sp = lax.axis_index("sp")
    tp = lax.axis_index("tp")
    has_next = sp < sp_count - 1
    has_prev = sp > 0
    order = list(range(CHUNKS))[::-1]

    def x_copy(c):
        part = pl.ds(c * chunk, chunk)
        return pltpu.make_async_copy(tokens.at[part], x0.at[part], x_sem.at[c])

    def w_copy(kind, layer):
        source = (wk_hbm, wv_hbm, wq_hbm, wo_hbm)[kind]
        target = (wk, wv, wq, wo)[kind]
        return pltpu.make_async_copy(
            source.at[layer], target.at[layer], w_sem.at[kind, layer]
        )

    def halo_copy(kind, layer, c):
        buffer = (kx, vx)[kind]
        return pltpu.make_async_remote_copy(
            src_ref=buffer.at[layer, pl.ds(reach + c * chunk, chunk)],
            dst_ref=buffer.at[layer, pl.ds(c * chunk, chunk)],
            send_sem=halo_send.at[kind, layer, c],
            recv_sem=halo_recv.at[kind, layer, c],
            device_id=(jnp.minimum(sp + 1, sp_count - 1), tp),
            device_id_type=MESH,
        )

    def pair_copy(layer, c):
        block = att.at[layer, tp, pl.ds(c * chunk, chunk)]
        return pltpu.make_async_remote_copy(
            src_ref=block,
            dst_ref=block,
            send_sem=pair_send.at[layer, c],
            recv_sem=pair_recv.at[layer, c],
            device_id=(sp, 1 - tp),
            device_id_type=MESH,
        )

    for c in order:
        x_copy(c).start()
    for kind in range(4):
        w_copy(kind, 0).start()

    barrier = pltpu.get_barrier_semaphore()
    pl.semaphore_signal(barrier, inc=1, device_id=(sp, 1 - tp), device_id_type=MESH)

    @pl.when(has_next)
    def _():
        pl.semaphore_signal(barrier, inc=1, device_id=(sp + 1, tp), device_id_type=MESH)

    @pl.when(has_prev)
    def _():
        pl.semaphore_signal(barrier, inc=1, device_id=(sp - 1, tp), device_id_type=MESH)

    @pl.when(jnp.logical_not(has_prev))
    def _():
        for layer in range(LAYERS):
            kx[layer, :reach, :] = jnp.zeros((reach, width), jnp.bfloat16)
            vx[layer, :reach, :] = jnp.zeros((reach, width), jnp.bfloat16)

    wide = bias.shape[2]
    size = padded.shape[1]
    padded[...] = jnp.zeros_like(padded)
    for layer in range(LAYERS):
        padded[layer * heads : (layer + 1) * heads, : table.shape[2]] = table[layer]
    place = lax.broadcasted_iota(jnp.int32, (size, wide), 1)
    source = lax.broadcasted_iota(jnp.int32, (size, wide), 0)
    onehot = (jnp.clip(band - 1 - place, -CLIP, CLIP) + CLIP == source).astype(jnp.float32)
    by_offset = jnp.dot(
        padded[...], onehot, precision=lax.Precision.HIGHEST, preferred_element_type=jnp.float32
    )
    for layer in range(LAYERS):
        for h in range(heads):
            line = by_offset[layer * heads + h : layer * heads + h + 1, :]
            skewed = pltpu.roll(
                jnp.broadcast_to(line, (SEG, wide)), wide - SEG + 1, 1, stride=1, stride_axis=0
            )
            bias[layer, h * SEG : (h + 1) * SEG, :] = skewed

    pl.semaphore_wait(
        barrier, 1 + has_next.astype(jnp.int32) + has_prev.astype(jnp.int32)
    )

    lane = lax.broadcasted_iota(jnp.int32, (1, width), 1)
    in_head = [
        (lane >= h * head_size) & (lane < (h + 1) * head_size) for h in range(heads)
    ]

    def project(hidden, layer, c, kind):
        part = slice(c * chunk, (c + 1) * chunk)
        weight = (wk, wv, wq)[kind]
        return jnp.dot(
            hidden[part, :], weight[layer], preferred_element_type=jnp.float32
        ).astype(jnp.bfloat16)

    def keys_values(hidden, layer, c):
        for kind in range(2):
            if c == order[0]:
                w_copy(kind, layer).wait()
            buffer = (kx, vx)[kind]
            buffer[layer, reach + c * chunk : reach + (c + 1) * chunk, :] = project(
                hidden, layer, c, kind
            )

            @pl.when(has_next)
            def _():
                halo_copy(kind, layer, c).start()

    def queries(hidden, layer, c):
        if c == order[0]:
            w_copy(2, layer).wait()
        part = slice(c * chunk, (c + 1) * chunk)
        query[part, :] = project(hidden, layer, c, 2) * jnp.bfloat16(head_size**-0.5)

    def attend(layer, c):
        @pl.when(has_prev)
        def _():
            halo_copy(0, layer, c).wait_recv()
            halo_copy(1, layer, c).wait_recv()

        column = lax.broadcasted_iota(jnp.int32, (1, band), 1)
        for seg in range(c * chunk // SEG, (c + 1) * chunk // SEG):
            block = query[seg * SEG : (seg + 1) * SEG, :]
            stacked = jnp.concatenate(
                [jnp.where(in_head[h], block, jnp.zeros_like(block)) for h in range(heads)],
                axis=0,
            )
            keys = kx[layer, seg * SEG : seg * SEG + band, :]
            values = vx[layer, seg * SEG : seg * SEG + band, :]
            scores = lax.dot_general(
                stacked, keys, (((1,), (1,)), ((), ())), preferred_element_type=jnp.float32
            )
            outside = (column < reach - seg * SEG) & jnp.logical_not(has_prev)
            scores = scores + bias[layer, :, :band]
            scores = jnp.where(outside, masked_score, scores)
            peak = jnp.max(scores, -1, keepdims=True)
            expo = jnp.exp(scores - peak)
            norm = jnp.sum(expo, -1, keepdims=True)
            mixed = jnp.dot(
                expo.astype(jnp.bfloat16), values, preferred_element_type=jnp.float32
            )
            mixed = mixed / norm
            own = jnp.zeros((SEG, width), jnp.float32)
            for h in range(heads):
                own = jnp.where(in_head[h], mixed[h * SEG : (h + 1) * SEG, :], own)
            att[layer, tp, seg * SEG : (seg + 1) * SEG, :] = own.astype(jnp.bfloat16)
        pair_copy(layer, c).start()

    def finish(hidden, layer, c):
        pair_copy(layer, c).wait_recv()
        if c == order[0]:
            w_copy(3, layer).wait()
        part = slice(c * chunk, (c + 1) * chunk)
        both = jnp.concatenate([att[layer, 0, part, :], att[layer, 1, part, :]], axis=1)
        total[...] = residual_scale * hidden[part, :].astype(jnp.float32) + jnp.dot(
            both, wo[layer], preferred_element_type=jnp.float32
        )
        step = 16
        for r in range(0, chunk, step):
            value = total[r : r + step, :]
            mean = jnp.sum(value, -1, keepdims=True) * (1.0 / model)
            centred = value - mean
            variance = jnp.sum(centred * centred, -1, keepdims=True) * (1.0 / model)
            scale = lax.rsqrt(variance + norm_eps)
            here = slice(c * chunk + r, c * chunk + r + step)
            if layer < LAYERS - 1:
                x1[here, :] = (
                    centred * scale * gain[layer : layer + 1, :] + shift[layer : layer + 1, :]
                ).astype(jnp.bfloat16)
            else:
                half = model // 2
                cols = pl.ds(pl.multiple_of(tp * half, half), half)
                out[here, :] = (
                    (total[r : r + step, cols] - mean) * scale * gain[layer : layer + 1, cols]
                    + shift[layer : layer + 1, cols]
                ).astype(jnp.bfloat16)

    for c in order:
        x_copy(c).wait()
        keys_values(x0, 0, c)
    for kind in range(4):
        w_copy(kind, 1).start()
    for c in order:
        queries(x0, 0, c)
    for c in order:
        attend(0, c)
        finish(x0, 0, c)
        keys_values(x1, 1, c)
        queries(x1, 1, c)
    for c in order:
        attend(1, c)
        finish(x1, 1, c)

    for layer in range(LAYERS):
        for c in order:
            pair_copy(layer, c).wait_send()

    @pl.when(has_next)
    def _():
        for layer in range(LAYERS):
            for c in order:
                for kind in range(2):
                    halo_copy(kind, layer, c).wait_send()


def body(
    sp_count, tokens, query_weight, key_weight, value_weight, out_weight, rel_table, norm_gain,
    norm_bias,
):
    rows, model = tokens.shape
    width = query_weight.shape[2]
    heads = rel_table.shape[1]
    reach = LEFT * SEG
    wide = -(-(reach + 2 * SEG - 1) // LANES) * LANES
    size = -(-rel_table.shape[2] // LANES) * LANES
    anywhere = pl.BlockSpec(memory_space=pl.ANY)
    vmem = pl.BlockSpec(memory_space=pltpu.VMEM)
    bf16 = jnp.bfloat16
    return pl.pallas_call(
        functools.partial(kernel, sp_count, heads),
        out_shape=jax.ShapeDtypeStruct((rows, model // 2), bf16),
        in_specs=[anywhere] * 5 + [vmem] * 3,
        out_specs=vmem,
        scratch_shapes=[
            pltpu.VMEM((rows, model), bf16),
            pltpu.VMEM((rows, model), bf16),
            pltpu.VMEM(query_weight.shape, bf16),
            pltpu.VMEM(key_weight.shape, bf16),
            pltpu.VMEM(value_weight.shape, bf16),
            pltpu.VMEM(out_weight.shape, bf16),
            pltpu.VMEM((rows, width), bf16),
            pltpu.VMEM((LAYERS, reach + rows, width), bf16),
            pltpu.VMEM((LAYERS, reach + rows, width), bf16),
            pltpu.VMEM((LAYERS, 2, rows, width), bf16),
            pltpu.VMEM((rows // CHUNKS, model), jnp.float32),
            pltpu.VMEM((LAYERS, heads * SEG, wide), jnp.float32),
            pltpu.VMEM((-(-LAYERS * heads // 8) * 8, size), jnp.float32),
            pltpu.SemaphoreType.DMA((CHUNKS,)),
            pltpu.SemaphoreType.DMA((4, LAYERS)),
            pltpu.SemaphoreType.DMA((2, LAYERS, CHUNKS)),
            pltpu.SemaphoreType.DMA((2, LAYERS, CHUNKS)),
            pltpu.SemaphoreType.DMA((LAYERS, CHUNKS)),
            pltpu.SemaphoreType.DMA((LAYERS, CHUNKS)),
        ],
        compiler_params=pltpu.CompilerParams(
            collective_id=0, has_side_effects=True, vmem_limit_bytes=48 * 1024 * 1024
        ),
    )(
        tokens, query_weight, key_weight, value_weight, out_weight, rel_table, norm_gain, norm_bias
    )


def solution(mesh):
    return jax.shard_map(
        functools.partial(body, mesh.shape["sp"]),
        mesh=mesh,
        in_specs=(
            P("sp", None),
            P(None, None, "tp"),
            P(None, None, "tp"),
            P(None, None, "tp"),
            P(),
            P(None, "tp", None),
            P(),
            P(),
        ),
        out_specs=P("sp", "tp"),
        check_vma=False,
    )
```

```python
import functools

import jax
import jax.numpy as jnp
from jax import lax
from jax.experimental import pallas as pl
from jax.experimental.pallas import tpu as pltpu
from jax.sharding import PartitionSpec as P

SEG = 64
LEFT = 4
CLIP = 128
LAYERS = 2
LANES = 128

residual_scale = 2.0**0.5
norm_eps = 1e-05
masked_score = -1e30
MESH = pl.DeviceIdType.MESH


def kernel(
    sp_count,
    heads,
    tokens,
    wq_hbm,
    wk_hbm,
    wv_hbm,
    wo_hbm,
    table_hbm,
    gain_hbm,
    shift_hbm,
    out,
    x0,
    x1,
    wq,
    wk,
    wv,
    wo,
    table,
    gain,
    shift,
    query,
    kx,
    vx,
    att,
    total,
    bias,
    padded,
    x_sem,
    w_sem,
    small_sem,
    halo_send,
    halo_recv,
    pair_send,
    pair_recv,
):
    rows, model = x0.shape
    width = query.shape[2]
    head_size = width // heads
    reach = LEFT * SEG
    band = reach + SEG
    segments = rows // SEG
    sp = lax.axis_index("sp")
    tp = lax.axis_index("tp")
    has_next = sp < sp_count - 1
    has_prev = sp > 0
    late = (segments // 2, segments)
    early = (0, segments // 2)

    def w_copy(kind, layer):
        source = (wk_hbm, wv_hbm, wq_hbm, wo_hbm)[kind]
        target = (wk, wv, wq, wo)[kind]
        return pltpu.make_async_copy(
            source.at[layer], target.at[layer], w_sem.at[kind, layer]
        )

    x_copy = pltpu.make_async_copy(tokens, x0, x_sem)
    small = [
        pltpu.make_async_copy(source, target, small_sem.at[index])
        for index, (source, target) in enumerate(
            ((table_hbm, table), (gain_hbm, gain), (shift_hbm, shift))
        )
    ]

    def halo_copy(kind, layer, seg):
        buffer = (kx, vx)[kind]
        return pltpu.make_async_remote_copy(
            src_ref=buffer.at[layer, pl.ds(reach + seg * SEG, SEG)],
            dst_ref=buffer.at[layer, pl.ds(seg * SEG, SEG)],
            send_sem=halo_send.at[kind, layer, seg],
            recv_sem=halo_recv.at[kind, layer, seg],
            device_id=(jnp.minimum(sp + 1, sp_count - 1), tp),
            device_id_type=MESH,
        )

    def pair_copy(layer, piece):
        first, last = piece
        block = att.at[layer, tp, pl.ds(first * SEG, (last - first) * SEG)]
        return pltpu.make_async_remote_copy(
            src_ref=block,
            dst_ref=block,
            send_sem=pair_send.at[layer, first],
            recv_sem=pair_recv.at[layer, first],
            device_id=(sp, 1 - tp),
            device_id_type=MESH,
        )

    x_copy.start()
    w_copy(0, 0).start()
    w_copy(1, 0).start()

    barrier = pltpu.get_barrier_semaphore()
    pl.semaphore_signal(barrier, inc=1, device_id=(sp, 1 - tp), device_id_type=MESH)

    @pl.when(has_next)
    def _():
        pl.semaphore_signal(barrier, inc=1, device_id=(sp + 1, tp), device_id_type=MESH)

    @pl.when(has_prev)
    def _():
        pl.semaphore_signal(barrier, inc=1, device_id=(sp - 1, tp), device_id_type=MESH)

    @pl.when(jnp.logical_not(has_prev))
    def _():
        for layer in range(LAYERS):
            kx[layer, :reach, :] = jnp.zeros((reach, width), jnp.bfloat16)
            vx[layer, :reach, :] = jnp.zeros((reach, width), jnp.bfloat16)

    lane = lax.broadcasted_iota(jnp.int32, (1, width), 1)
    in_head = [
        (lane >= h * head_size) & (lane < (h + 1) * head_size) for h in range(heads)
    ]

    def build_bias():
        wide = bias.shape[2]
        size = padded.shape[1]
        padded[...] = jnp.zeros_like(padded)
        for layer in range(LAYERS):
            padded[layer * heads : (layer + 1) * heads, : table.shape[2]] = table[layer]
        place = lax.broadcasted_iota(jnp.int32, (size, wide), 1)
        source = lax.broadcasted_iota(jnp.int32, (size, wide), 0)
        onehot = (jnp.clip(band - 1 - place, -CLIP, CLIP) + CLIP == source).astype(jnp.float32)
        by_offset = jnp.dot(
            padded[...],
            onehot,
            precision=lax.Precision.HIGHEST,
            preferred_element_type=jnp.float32,
        )
        for layer in range(LAYERS):
            for h in range(heads):
                line = by_offset[layer * heads + h : layer * heads + h + 1, :]
                skewed = pltpu.roll(
                    jnp.broadcast_to(line, (SEG, wide)), wide - SEG + 1, 1, stride=1, stride_axis=0
                )
                bias[layer, h * SEG : (h + 1) * SEG, :] = skewed

    def project(hidden, layer, piece, kind):
        part = slice(piece[0] * SEG, piece[1] * SEG)
        weight = (wk, wv, wq)[kind]
        return jnp.dot(
            hidden[part, :], weight[layer], preferred_element_type=jnp.float32
        ).astype(jnp.bfloat16)

    def keys(hidden, layer, piece):
        part = slice(reach + piece[0] * SEG, reach + piece[1] * SEG)
        kx[layer, part, :] = project(hidden, layer, piece, 0)

        @pl.when(has_next)
        def _():
            halo_copy(0, layer, piece[1] - 1).start()

    def values(hidden, layer, piece):
        part = slice(reach + piece[0] * SEG, reach + piece[1] * SEG)
        vx[layer, part, :] = project(hidden, layer, piece, 1)

        @pl.when(has_next)
        def _():
            halo_copy(1, layer, piece[1] - 1).start()
            for seg in range(piece[0], piece[1] - 1)[::-1]:
                halo_copy(0, layer, seg).start()
                halo_copy(1, layer, seg).start()

    def queries(hidden, layer, piece):
        part = slice(piece[0] * SEG, piece[1] * SEG)
        query[layer, part, :] = project(hidden, layer, piece, 2) * jnp.bfloat16(head_size**-0.5)

    def attend(layer, seg):
        @pl.when(has_prev)
        def _():
            halo_copy(0, layer, seg).wait_recv()
            halo_copy(1, layer, seg).wait_recv()

        column = lax.broadcasted_iota(jnp.int32, (1, band), 1)
        block = query[layer, seg * SEG : (seg + 1) * SEG, :]
        stacked = jnp.concatenate(
            [jnp.where(in_head[h], block, jnp.zeros_like(block)) for h in range(heads)], axis=0
        )
        key_band = kx[layer, seg * SEG : seg * SEG + band, :]
        value_band = vx[layer, seg * SEG : seg * SEG + band, :]
        scores = lax.dot_general(
            stacked, key_band, (((1,), (1,)), ((), ())), preferred_element_type=jnp.float32
        )
        outside = (column < reach - seg * SEG) & jnp.logical_not(has_prev)
        scores = jnp.where(outside, masked_score, scores + bias[layer, :, :band])
        peak = jnp.max(scores, -1, keepdims=True)
        expo = jnp.exp(scores - peak)
        norm = jnp.sum(expo, -1, keepdims=True)
        mixed = jnp.dot(
            expo.astype(jnp.bfloat16), value_band, preferred_element_type=jnp.float32
        )
        mixed = mixed * (1.0 / norm)
        own = mixed[:SEG, :]
        for h in range(1, heads):
            own = jnp.where(in_head[h], mixed[h * SEG : (h + 1) * SEG, :], own)
        att[layer, tp, seg * SEG : (seg + 1) * SEG, :] = own.astype(jnp.bfloat16)

    def finish(hidden, layer, piece):
        part = slice(piece[0] * SEG, piece[1] * SEG)
        count = (piece[1] - piece[0]) * SEG

        def half(owner):
            weight = wo[layer, pl.ds(pl.multiple_of(owner * width, width), width), :]
            return jnp.dot(att[layer, owner, part, :], weight, preferred_element_type=jnp.float32)

        total[:count, :] = half(tp)
        pair_copy(layer, piece).wait_recv()
        total[:count, :] += half(1 - tp)
        step = 16
        for r in range(0, count, step):
            here = slice(piece[0] * SEG + r, piece[0] * SEG + r + step)
            value = total[r : r + step, :] + residual_scale * hidden[here, :].astype(jnp.float32)
            mean = jnp.sum(value, -1, keepdims=True) * (1.0 / model)
            centred = value - mean
            variance = jnp.sum(centred * centred, -1, keepdims=True) * (1.0 / model)
            scale = lax.rsqrt(variance + norm_eps)
            if layer < LAYERS - 1:
                x1[here, :] = (
                    centred * scale * gain[layer : layer + 1, :] + shift[layer : layer + 1, :]
                ).astype(jnp.bfloat16)
            else:
                cols = pl.ds(pl.multiple_of(tp * (model // 2), model // 2), model // 2)
                value = total[r : r + step, cols] + residual_scale * hidden[here, cols].astype(
                    jnp.float32
                )
                out[here, :] = (
                    (value - mean) * scale * gain[layer : layer + 1, cols]
                    + shift[layer : layer + 1, cols]
                ).astype(jnp.bfloat16)

    every = (0, segments)
    x_copy.wait()
    w_copy(0, 0).wait()
    for copy in (w_copy(2, 0), w_copy(3, 0), *small):
        copy.start()
    pl.semaphore_wait(barrier, 1 + has_next.astype(jnp.int32) + has_prev.astype(jnp.int32))
    keys(x0, 0, every)
    w_copy(1, 0).wait()
    values(x0, 0, every)
    w_copy(2, 0).wait()
    queries(x0, 0, every)
    for kind in range(4):
        w_copy(kind, 1).start()
    for copy in small:
        copy.wait()
    build_bias()
    w_copy(3, 0).wait()
    for kind in range(4):
        w_copy(kind, 1).wait()

    for seg in range(*late)[::-1]:
        attend(0, seg)
    pair_copy(0, late).start()
    for seg in range(early[0] + 1, early[1])[::-1]:
        attend(0, seg)
    finish(x0, 0, late)
    keys(x1, 1, late)
    values(x1, 1, late)
    attend(0, 0)
    pair_copy(0, early).start()
    queries(x1, 1, late)
    finish(x0, 0, early)
    keys(x1, 1, early)
    values(x1, 1, early)
    queries(x1, 1, early)

    for seg in range(*late)[::-1]:
        attend(1, seg)
    pair_copy(1, late).start()
    pieces = [(seg, seg + 1) for seg in range(*early)[::-1]]
    waiting = late
    for piece in pieces:
        attend(1, piece[0])
        pair_copy(1, piece).start()
        finish(x1, 1, waiting)
        waiting = piece
    finish(x1, 1, waiting)

    for layer, piece in [(0, late), (0, early), (1, late)] + [(1, piece) for piece in pieces]:
        pair_copy(layer, piece).wait_send()

    @pl.when(has_next)
    def _():
        for layer in range(LAYERS):
            for seg in range(segments):
                for kind in range(2):
                    halo_copy(kind, layer, seg).wait_send()


def body(
    sp_count, tokens, query_weight, key_weight, value_weight, out_weight, rel_table, norm_gain,
    norm_bias,
):
    rows, model = tokens.shape
    width = query_weight.shape[2]
    heads = rel_table.shape[1]
    reach = LEFT * SEG
    segments = rows // SEG
    wide = -(-(reach + 2 * SEG - 1) // LANES) * LANES
    size = -(-rel_table.shape[2] // LANES) * LANES
    hbm = pl.BlockSpec(memory_space=pltpu.MemorySpace.HBM)
    vmem = pl.BlockSpec(memory_space=pltpu.VMEM)
    bf16 = jnp.bfloat16
    return pl.pallas_call(
        functools.partial(kernel, sp_count, heads),
        out_shape=jax.ShapeDtypeStruct((rows, model // 2), bf16),
        in_specs=[hbm] * 8,
        out_specs=vmem,
        scratch_shapes=[
            pltpu.VMEM((rows, model), bf16),
            pltpu.VMEM((rows, model), bf16),
            pltpu.VMEM(query_weight.shape, bf16),
            pltpu.VMEM(key_weight.shape, bf16),
            pltpu.VMEM(value_weight.shape, bf16),
            pltpu.VMEM(out_weight.shape, bf16),
            pltpu.VMEM(rel_table.shape, jnp.float32),
            pltpu.VMEM(norm_gain.shape, jnp.float32),
            pltpu.VMEM(norm_bias.shape, jnp.float32),
            pltpu.VMEM((LAYERS, rows, width), bf16),
            pltpu.VMEM((LAYERS, reach + rows, width), bf16),
            pltpu.VMEM((LAYERS, reach + rows, width), bf16),
            pltpu.VMEM((LAYERS, 2, rows, width), bf16),
            pltpu.VMEM((rows // 2, model), jnp.float32),
            pltpu.VMEM((LAYERS, heads * SEG, wide), jnp.float32),
            pltpu.VMEM((-(-LAYERS * heads // 8) * 8, size), jnp.float32),
            pltpu.SemaphoreType.DMA,
            pltpu.SemaphoreType.DMA((4, LAYERS)),
            pltpu.SemaphoreType.DMA((3,)),
            pltpu.SemaphoreType.DMA((2, LAYERS, segments)),
            pltpu.SemaphoreType.DMA((2, LAYERS, segments)),
            pltpu.SemaphoreType.DMA((LAYERS, segments)),
            pltpu.SemaphoreType.DMA((LAYERS, segments)),
        ],
        compiler_params=pltpu.CompilerParams(
            collective_id=0, has_side_effects=True, vmem_limit_bytes=65950000
        ),
    )(
        tokens, query_weight, key_weight, value_weight, out_weight, rel_table, norm_gain, norm_bias
    )


def solution(mesh):
    return jax.shard_map(
        functools.partial(body, mesh.shape["sp"]),
        mesh=mesh,
        in_specs=(
            P("sp", None),
            P(None, None, "tp"),
            P(None, None, "tp"),
            P(None, None, "tp"),
            P(),
            P(None, "tp", None),
            P(),
            P(),
        ),
        out_specs=P("sp", "tp"),
        check_vma=False,
    )
```

```python
import functools

import jax
import jax.numpy as jnp
from jax import lax
from jax.experimental import pallas as pl
from jax.experimental.pallas import tpu as pltpu
from jax.sharding import PartitionSpec as P

SEG = 64
LEFT = 4
CLIP = 128
LAYERS = 2
LANES = 128

residual_scale = 2.0**0.5
norm_eps = 1e-05
masked_score = -1e30
MESH = pl.DeviceIdType.MESH


def kernel(
    sp_count,
    heads,
    tokens,
    wq_hbm,
    wk_hbm,
    wv_hbm,
    wo_hbm,
    table_hbm,
    gain_hbm,
    shift_hbm,
    out,
    x0,
    x1,
    wq,
    wk,
    wv,
    wo,
    table,
    gain,
    shift,
    query,
    kx,
    vx,
    att,
    total,
    bias,
    padded,
    x_sem,
    w_sem,
    small_sem,
    halo_send,
    halo_recv,
    pair_send,
    pair_recv,
):
    rows, model = x0.shape
    width = query.shape[2]
    head_size = width // heads
    reach = LEFT * SEG
    band = reach + SEG
    segments = rows // SEG
    sp = lax.axis_index("sp")
    tp = lax.axis_index("tp")
    has_next = sp < sp_count - 1
    has_prev = sp > 0
    late = (segments // 2, segments)
    early = (0, segments // 2)

    def w_copy(kind, layer):
        source = (wk_hbm, wv_hbm, wq_hbm, wo_hbm)[kind]
        target = (wk, wv, wq, wo)[kind]
        return pltpu.make_async_copy(
            source.at[layer], target.at[layer], w_sem.at[kind, layer]
        )

    x_copy = pltpu.make_async_copy(tokens, x0, x_sem)
    small = [
        pltpu.make_async_copy(source, target, small_sem.at[index])
        for index, (source, target) in enumerate(
            ((table_hbm, table), (gain_hbm, gain), (shift_hbm, shift))
        )
    ]

    def halo_copy(kind, layer, seg):
        buffer = (kx, vx)[kind]
        return pltpu.make_async_remote_copy(
            src_ref=buffer.at[layer, pl.ds(reach + seg * SEG, SEG)],
            dst_ref=buffer.at[layer, pl.ds(seg * SEG, SEG)],
            send_sem=halo_send.at[kind, layer, seg],
            recv_sem=halo_recv.at[kind, layer, seg],
            device_id=(jnp.minimum(sp + 1, sp_count - 1), tp),
            device_id_type=MESH,
        )

    def pair_copy(layer, piece):
        first, last = piece
        block = att.at[layer, tp, pl.ds(first * SEG, (last - first) * SEG)]
        return pltpu.make_async_remote_copy(
            src_ref=block,
            dst_ref=block,
            send_sem=pair_send.at[layer, first],
            recv_sem=pair_recv.at[layer, first],
            device_id=(sp, 1 - tp),
            device_id_type=MESH,
        )

    x_copy.start()
    w_copy(0, 0).start()
    w_copy(1, 0).start()

    barrier = pltpu.get_barrier_semaphore()
    pl.semaphore_signal(barrier, inc=1, device_id=(sp, 1 - tp), device_id_type=MESH)

    @pl.when(has_next)
    def _():
        pl.semaphore_signal(barrier, inc=1, device_id=(sp + 1, tp), device_id_type=MESH)

    @pl.when(has_prev)
    def _():
        pl.semaphore_signal(barrier, inc=1, device_id=(sp - 1, tp), device_id_type=MESH)

    @pl.when(jnp.logical_not(has_prev))
    def _():
        for layer in range(LAYERS):
            kx[layer, :reach, :] = jnp.zeros((reach, width), jnp.bfloat16)
            vx[layer, :reach, :] = jnp.zeros((reach, width), jnp.bfloat16)

    lane = lax.broadcasted_iota(jnp.int32, (1, width), 1)
    in_head = [
        (lane >= h * head_size) & (lane < (h + 1) * head_size) for h in range(heads)
    ]

    def build_bias():
        wide = bias.shape[2]
        size = padded.shape[1]
        padded[...] = jnp.zeros_like(padded)
        for layer in range(LAYERS):
            padded[layer * heads : (layer + 1) * heads, : table.shape[2]] = table[layer]
        place = lax.broadcasted_iota(jnp.int32, (size, wide), 1)
        source = lax.broadcasted_iota(jnp.int32, (size, wide), 0)
        onehot = (jnp.clip(band - 1 - place, -CLIP, CLIP) + CLIP == source).astype(jnp.float32)
        by_offset = jnp.dot(
            padded[...],
            onehot,
            precision=lax.Precision.HIGHEST,
            preferred_element_type=jnp.float32,
        )
        for layer in range(LAYERS):
            for h in range(heads):
                line = by_offset[layer * heads + h : layer * heads + h + 1, :]
                skewed = pltpu.roll(
                    jnp.broadcast_to(line, (SEG, wide)), wide - SEG + 1, 1, stride=1, stride_axis=0
                )
                bias[layer, h * SEG : (h + 1) * SEG, :] = skewed

    def project(hidden, layer, piece, kind):
        part = slice(piece[0] * SEG, piece[1] * SEG)
        weight = (wk, wv, wq)[kind]
        return jnp.dot(
            hidden[part, :], weight[layer], preferred_element_type=jnp.float32
        ).astype(jnp.bfloat16)

    def keys(hidden, layer, piece):
        part = slice(reach + piece[0] * SEG, reach + piece[1] * SEG)
        kx[layer, part, :] = project(hidden, layer, piece, 0)

        @pl.when(has_next)
        def _():
            halo_copy(0, layer, piece[1] - 1).start()

    def values(hidden, layer, piece):
        part = slice(reach + piece[0] * SEG, reach + piece[1] * SEG)
        vx[layer, part, :] = project(hidden, layer, piece, 1)

        @pl.when(has_next)
        def _():
            halo_copy(1, layer, piece[1] - 1).start()
            for seg in range(piece[0], piece[1] - 1)[::-1]:
                halo_copy(0, layer, seg).start()
                halo_copy(1, layer, seg).start()

    def queries(hidden, layer, piece):
        part = slice(piece[0] * SEG, piece[1] * SEG)
        query[layer, part, :] = project(hidden, layer, piece, 2) * jnp.bfloat16(head_size**-0.5)

    def attend(layer, seg):
        @pl.when(has_prev)
        def _():
            halo_copy(0, layer, seg).wait_recv()
            halo_copy(1, layer, seg).wait_recv()

        column = lax.broadcasted_iota(jnp.int32, (1, band), 1)
        block = query[layer, seg * SEG : (seg + 1) * SEG, :]
        stacked = jnp.concatenate(
            [jnp.where(in_head[h], block, jnp.zeros_like(block)) for h in range(heads)], axis=0
        )
        key_band = kx[layer, seg * SEG : seg * SEG + band, :]
        value_band = vx[layer, seg * SEG : seg * SEG + band, :]
        scores = lax.dot_general(
            stacked, key_band, (((1,), (1,)), ((), ())), preferred_element_type=jnp.float32
        )
        outside = (column < reach - seg * SEG) & jnp.logical_not(has_prev)
        scores = jnp.where(outside, masked_score, scores + bias[layer, :, :band])
        peak = jnp.max(scores, -1, keepdims=True)
        expo = jnp.exp(scores - peak)
        norm = jnp.sum(expo, -1, keepdims=True)
        mixed = jnp.dot(
            expo.astype(jnp.bfloat16), value_band, preferred_element_type=jnp.float32
        )
        mixed = mixed * (1.0 / norm)
        own = mixed[:SEG, :]
        for h in range(1, heads):
            own = jnp.where(in_head[h], mixed[h * SEG : (h + 1) * SEG, :], own)
        att[layer, tp, seg * SEG : (seg + 1) * SEG, :] = own.astype(jnp.bfloat16)

    def finish(hidden, layer, piece):
        part = slice(piece[0] * SEG, piece[1] * SEG)
        count = (piece[1] - piece[0]) * SEG

        def half(owner):
            weight = wo[layer, pl.ds(pl.multiple_of(owner * width, width), width), :]
            return jnp.dot(att[layer, owner, part, :], weight, preferred_element_type=jnp.float32)

        total[:count, :] = half(tp) + residual_scale * hidden[part, :].astype(jnp.float32)
        pair_copy(layer, piece).wait_recv()
        total[:count, :] += half(1 - tp)
        step = 16
        for r in range(0, count, step):
            here = slice(piece[0] * SEG + r, piece[0] * SEG + r + step)
            value = total[r : r + step, :]
            mean = jnp.sum(value, -1, keepdims=True) * (1.0 / model)
            centred = value - mean
            variance = jnp.sum(centred * centred, -1, keepdims=True) * (1.0 / model)
            scale = lax.rsqrt(variance + norm_eps)
            if layer < LAYERS - 1:
                x1[here, :] = (
                    centred * scale * gain[layer : layer + 1, :] + shift[layer : layer + 1, :]
                ).astype(jnp.bfloat16)
            else:
                cols = pl.ds(pl.multiple_of(tp * (model // 2), model // 2), model // 2)
                out[here, :] = (
                    (total[r : r + step, cols] - mean) * scale * gain[layer : layer + 1, cols]
                    + shift[layer : layer + 1, cols]
                ).astype(jnp.bfloat16)

    every = (0, segments)
    x_copy.wait()
    w_copy(0, 0).wait()
    for copy in (w_copy(2, 0), w_copy(3, 0), *small):
        copy.start()
    pl.semaphore_wait(barrier, 1 + has_next.astype(jnp.int32) + has_prev.astype(jnp.int32))
    keys(x0, 0, every)
    w_copy(1, 0).wait()
    values(x0, 0, every)
    w_copy(2, 0).wait()
    queries(x0, 0, every)
    for kind in range(4):
        w_copy(kind, 1).start()
    for copy in small:
        copy.wait()
    build_bias()
    w_copy(3, 0).wait()

    for seg in range(*late)[::-1]:
        attend(0, seg)
    pair_copy(0, late).start()
    for seg in range(early[0] + 1, early[1])[::-1]:
        attend(0, seg)
    finish(x0, 0, late)
    w_copy(0, 1).wait()
    w_copy(1, 1).wait()
    keys(x1, 1, late)
    values(x1, 1, late)
    attend(0, 0)
    pair_copy(0, early).start()
    w_copy(2, 1).wait()
    w_copy(3, 1).wait()
    queries(x1, 1, late)
    finish(x0, 0, early)
    keys(x1, 1, early)
    values(x1, 1, early)
    queries(x1, 1, early)

    for seg in range(*late)[::-1]:
        attend(1, seg)
    pair_copy(1, late).start()
    pieces = [(seg, seg + 1) for seg in range(*early)[::-1]]
    waiting = late
    for piece in pieces:
        attend(1, piece[0])
        pair_copy(1, piece).start()
        finish(x1, 1, waiting)
        waiting = piece
    finish(x1, 1, waiting)

    for layer, piece in [(0, late), (0, early), (1, late)] + [(1, piece) for piece in pieces]:
        pair_copy(layer, piece).wait_send()

    @pl.when(has_next)
    def _():
        for layer in range(LAYERS):
            for seg in range(segments):
                for kind in range(2):
                    halo_copy(kind, layer, seg).wait_send()


def body(
    sp_count, tokens, query_weight, key_weight, value_weight, out_weight, rel_table, norm_gain,
    norm_bias,
):
    rows, model = tokens.shape
    width = query_weight.shape[2]
    heads = rel_table.shape[1]
    reach = LEFT * SEG
    segments = rows // SEG
    wide = -(-(reach + 2 * SEG - 1) // LANES) * LANES
    size = -(-rel_table.shape[2] // LANES) * LANES
    hbm = pl.BlockSpec(memory_space=pltpu.MemorySpace.HBM)
    vmem = pl.BlockSpec(memory_space=pltpu.VMEM)
    bf16 = jnp.bfloat16
    return pl.pallas_call(
        functools.partial(kernel, sp_count, heads),
        out_shape=jax.ShapeDtypeStruct((rows, model // 2), bf16),
        in_specs=[hbm] * 8,
        out_specs=vmem,
        scratch_shapes=[
            pltpu.VMEM((rows, model), bf16),
            pltpu.VMEM((rows, model), bf16),
            pltpu.VMEM(query_weight.shape, bf16),
            pltpu.VMEM(key_weight.shape, bf16),
            pltpu.VMEM(value_weight.shape, bf16),
            pltpu.VMEM(out_weight.shape, bf16),
            pltpu.VMEM(rel_table.shape, jnp.float32),
            pltpu.VMEM(norm_gain.shape, jnp.float32),
            pltpu.VMEM(norm_bias.shape, jnp.float32),
            pltpu.VMEM((LAYERS, rows, width), bf16),
            pltpu.VMEM((LAYERS, reach + rows, width), bf16),
            pltpu.VMEM((LAYERS, reach + rows, width), bf16),
            pltpu.VMEM((LAYERS, 2, rows, width), bf16),
            pltpu.VMEM((rows // 2, model), jnp.float32),
            pltpu.VMEM((LAYERS, heads * SEG, wide), jnp.float32),
            pltpu.VMEM((-(-LAYERS * heads // 8) * 8, size), jnp.float32),
            pltpu.SemaphoreType.DMA,
            pltpu.SemaphoreType.DMA((4, LAYERS)),
            pltpu.SemaphoreType.DMA((3,)),
            pltpu.SemaphoreType.DMA((2, LAYERS, segments)),
            pltpu.SemaphoreType.DMA((2, LAYERS, segments)),
            pltpu.SemaphoreType.DMA((LAYERS, segments)),
            pltpu.SemaphoreType.DMA((LAYERS, segments)),
        ],
        compiler_params=pltpu.CompilerParams(
            collective_id=0, has_side_effects=True, vmem_limit_bytes=56000000
        ),
    )(
        *(
            pltpu.with_memory_space_constraint(operand, pltpu.MemorySpace.HBM)
            for operand in (
                tokens,
                query_weight,
                key_weight,
                value_weight,
                out_weight,
                rel_table,
                norm_gain,
                norm_bias,
            )
        )
    )


def solution(mesh):
    return jax.shard_map(
        functools.partial(body, mesh.shape["sp"]),
        mesh=mesh,
        in_specs=(
            P("sp", None),
            P(None, None, "tp"),
            P(None, None, "tp"),
            P(None, None, "tp"),
            P(),
            P(None, "tp", None),
            P(),
            P(),
        ),
        out_specs=P("sp", "tp"),
        check_vma=False,
    )
```
